32 devices in a mesh: rep: 8 (over z, y), fs: 2 (over core), tp: 2 (over x).
Axes of the slice: x: 2, y: 2, z: 4, core: 2. Of those that a mesh axis runs over, the one named last changes fastest.
Arguments:
- inputs: bfloat16 [2048, 2048], P(('rep', 'fs'), 'tp'), may hold values from -6 to 6
- cotangent: bfloat16 [2048, 2048], P(('rep', 'fs'), 'tp'), may hold values from -6 to 6
- w_up: bfloat16 [2048, 4096], P('fs', 'tp'), may hold values from -0.125 to 0.125
- w_down: bfloat16 [4096, 2048], P('tp', 'fs'), may hold values from -0.09375 to 0.09375
Outputs:
- grad_inputs: bfloat16 [2048, 2048], P(('rep', 'fs'), 'tp')
- grad_up: float32 [2048, 4096], P('fs', 'tp')
- grad_down: float32 [4096, 2048], P('tp', 'fs')
The draws below stay inside these ranges and needn't reach their ends.
All inputs are finite; a program needn't handle non-finite values.
Results may differ from the reference program's by a relative error of at most 0.011.
Values may be sent and summed in bfloat16 or wider, within the bound.
A program may use at most 128 MiB of HBM per device.

```python
import jax
import jax.numpy as jnp
from jax import lax

D = 2048
FF = 4096
TOKENS = 2048
N_TP = 2


def raised(entries, key, source, target, parts, factor):
    owner, partner = [(jnp.arange(entries.shape[axis_at]) // (entries.shape[axis_at] // parts)).reshape([-1 if axis == axis_at else 1 for axis in range(entries.ndim)]) for axis_at in (source, target)]
    chosen = jax.random.permutation(key, parts)[partner]
    strong = (owner == chosen) | (owner == (partner + parts // 2) % parts)
    return jnp.where(strong, factor * entries, entries)


def levels(own_key, shape, pieces, low, largest):
    def one(position, shards_of):
        heights = jax.random.uniform(jax.random.fold_in(jax.random.fold_in(own_key, 6), position), (shards_of,), jnp.float32, low / len(pieces), largest / len(pieces))
        return jnp.repeat(jnp.exp(heights), shape[position] // shards_of).reshape((-1,) + (1,) * (len(shape) - position - 1))

    loudness = one(*pieces[0])
    for cut in pieces[1:]:
        loudness = loudness * one(*cut)
    return loudness


def normal_values(rng, shape, width, most, split=(), dtype=jnp.bfloat16):
    entries = jax.random.normal(rng, shape, jnp.float32) * width
    if len(split) > 0:
        entries = levels(rng, shape, split, -0.22, 0.18) * entries
    return jnp.clip(entries, min=-most, max=most).astype(dtype)


def bell_draw_with(rng, extent, deviation, limit, cuts, heavy, dtype=jnp.bfloat16):
    values = deviation * jax.random.normal(rng, extent, jnp.float32)
    if cuts:
        values = values * levels(rng, extent, cuts, -0.22, 0.18)
    return jnp.clip(raised(values, jax.random.fold_in(rng, 3), *heavy), -limit, limit).astype(dtype)


def setup_inputs(seed: int = 0) -> dict:
    arg_keys = jax.random.split(jax.random.key(seed), 5)
    return {
        "inputs": bell_draw_with(arg_keys[0], (TOKENS, D), 1.0, 6.0, ((0, 16), (1, 2)), (0, 1, 16, 2.0)),
        "cotangent": bell_draw_with(arg_keys[1], (TOKENS, D), 1.0, 6.0, ((0, 16), (1, 2)), (0, 1, 16, 2.0)),
        "w_up": normal_values(arg_keys[2], (D, FF), D ** -0.5, 0.125, ((0, 2), (1, 2))),
        "w_down": normal_values(arg_keys[3], (FF, D), FF ** -0.5, 0.09375, ((0, 2), (1, 2))),
    }


def reference(inputs, cotangent, w_up, w_down):
    preact = jnp.dot(inputs, w_up, preferred_element_type=jnp.float32)
    relu_pre = jnp.maximum(preact, 0.0)
    squared = (relu_pre * relu_pre).astype(jnp.bfloat16)
    act_grad = jnp.dot(cotangent, w_down.T, preferred_element_type=jnp.float32)
    pre_grad = (2.0 * relu_pre * act_grad).astype(jnp.bfloat16)
    grad_up = jnp.dot(inputs.T, pre_grad, preferred_element_type=jnp.float32)
    grad_down = jnp.dot(squared.T, cotangent, preferred_element_type=jnp.float32)
    group = w_up.shape[1] // N_TP
    total = jnp.zeros(inputs.shape, jnp.float32)
    for index in range(N_TP):
        partial_value = jnp.dot(pre_grad[:, index * group:(index + 1) * group],
                          w_up[:, index * group:(index + 1) * group].T,
                          preferred_element_type=jnp.float32).astype(jnp.bfloat16)
        partial_value = lax.optimization_barrier(partial_value)
        total = total + partial_value.astype(jnp.float32)
    return total.astype(jnp.bfloat16), grad_up, grad_down
```

```python
import functools

import jax
import jax.numpy as jnp
from jax import lax
from jax.experimental import pallas as pl
from jax.experimental.pallas import tpu as pltpu
from jax.sharding import PartitionSpec as P

MESH = pl.DeviceIdType.MESH
X, Y, UP, DOWN = range(4)
PAIR = 2
OWN, SIBLING, OTHER = range(3)
PLACES = (0, 1, 2, 3, 0, 1, 4, 5)
GRANT = 22 * 1024 * 1024


def contract_rows(left, right):
    return lax.dot_general(
        left, right, (((0,), (0,)), ((), ())), preferred_element_type=jnp.float32
    )


def contract_cols(left, right):
    return lax.dot_general(
        left, right, (((1,), (1,)), ((), ())), preferred_element_type=jnp.float32
    )


def nearest(z, depth, index):
    near = jnp.minimum(z, depth - 1 - z)
    away = (index + 1) // 2
    around = z - away if index % 2 else z + away
    outward = jnp.where(z < depth - 1 - z, z + (index - near), z - (index - near))
    return jnp.where(index <= 2 * near, around, outward)


def hidden_kernel(reps, x_ref, c_ref, up_ref, down_ref,
                  acc_up, acc_down, gx, gc, pg, sq, mine, theirs,
                  up, down, stage, sent,
                  free_sem, send_sem, recv_sem, swap_sem, turn_sem, own_sem, stage_sem,
                  pair_send, pair_recv, part_sem):
    rep, fs, tp = lax.axis_index("rep"), lax.axis_index("fs"), lax.axis_index("tp")
    z, y = rep // PAIR, rep % PAIR
    depth = reps // PAIR
    height, width = x_ref.shape
    half = height // 2
    hidden = up.shape[2]
    reach = depth - 2
    target = {
        X: {"tp": 1 - tp},
        Y: {"rep": z * PAIR + (1 - y)},
        UP: {"rep": jnp.minimum(z + 1, depth - 1) * PAIR + y},
        DOWN: {"rep": jnp.maximum(z - 1, 0) * PAIR + y},
    }
    sibling = {"fs": 1 - fs}
    above, below = z < depth - 1, z > 0
    planes = [nearest(z, depth, index) for index in range(depth)]
    own_block = ((tp + fs) % 2) * OTHER

    chunk = stage.shape[1]
    chunks = down_ref.shape[0] // chunk

    def stage_copy(number):
        rows = pl.ds(number * chunk, chunk)
        return pltpu.make_async_copy(down_ref.at[rows], stage.at[number % 2], stage_sem.at[number % 2])

    owns = [
        pltpu.make_async_copy(x_ref, gx.at[rep, own_block], own_sem.at[0]),
        pltpu.make_async_copy(c_ref, gc.at[rep, own_block], own_sem.at[1]),
    ]
    for own in owns:
        own.start()
    stage_copy(0).start()
    stage_copy(1).start()
    own_up = pltpu.make_async_copy(up_ref, up.at[0], own_sem.at[2])
    own_up.start()

    barrier = pltpu.get_barrier_semaphore()

    def greet(device):
        pl.semaphore_signal(barrier, inc=1, device_id=device, device_id_type=MESH)

    greet(target[X])
    greet(target[Y])
    greet(sibling)
    pl.when(above)(lambda: greet(target[UP]))
    pl.when(below)(lambda: greet(target[DOWN]))
    pl.semaphore_wait(barrier, 3 + above.astype(jnp.int32) + below.astype(jnp.int32))

    started = []

    def copy(way, sub, at):
        at_z, at_y, at_t = at
        array, part = sub
        unit = at_z * PAIR + at_y
        place = (gx, gc)[array].at[unit, ((at_t + fs) % 2) * OTHER, pl.ds(part * half, half)]
        index, piece = array * 2 + part, unit * 2 + at_t
        return pltpu.make_async_remote_copy(
            src_ref=place, dst_ref=place,
            send_sem=send_sem.at[way, index, piece], recv_sem=recv_sem.at[index, piece],
            device_id=target[way], device_id_type=MESH,
        )

    def start(way, sub, at, condition=None):
        if condition is None:
            copy(way, sub, at).start()
        else:
            pl.when(condition)(lambda: copy(way, sub, at).start())
        started.append((way, sub, at, condition))

    def arrive(sub, at, condition=None):
        if condition is None:
            copy(X, sub, at).wait_recv()
        else:
            pl.when(condition)(lambda: copy(X, sub, at).wait_recv())

    first = [(array, 0) for array in range(2)]
    second = [(array, 1) for array in range(2)]
    subs = first + second
    far_y, far_x = subs[:3], subs[3:]

    def sides(distance):
        return (
            (z - distance, z >= distance, UP, jnp.logical_and(z >= distance, above)),
            (z + distance, z + distance < depth, DOWN, jnp.logical_and(z + distance < depth, below)),
        )

    def column(distance, sub):
        for at_z, there, way, onward in sides(distance):
            at = (at_z, y, tp)
            arrive(sub, at, there)
            start(way, sub, at, onward)
            start(X, sub, at, there)
            start(Y, sub, at, there)

    def cross(one, two):
        arrive(one, (z, y, 1 - tp))
        start(Y, one, (z, y, 1 - tp))
        arrive(two, (z, 1 - y, tp))
        start(X, two, (z, 1 - y, tp))

    def corner_own(sub):
        at = (z, 1 - y, 1 - tp)
        arrive(sub, at)
        start(UP, sub, at, above)
        start(DOWN, sub, at, below)

    def corner(distance, sub):
        for at_z, there, way, onward in sides(distance):
            at = (at_z, 1 - y, 1 - tp)
            arrive(sub, at, there)
            if distance < reach:
                start(way, sub, at, onward)

    last = planes[depth - 1]
    far = jnp.logical_or(last - z > reach, z - last > reach)

    def far_cross(sub):
        if sub in far_y:
            arrive(sub, (last, y, 1 - tp))
            start(Y, sub, (last, y, 1 - tp), far)
        else:
            arrive(sub, (last, 1 - y, tp))
            start(X, sub, (last, 1 - y, tp), far)

    def unit_of(index, row):
        return planes[index] * PAIR + row

    turns = [(0, y), (0, 1 - y), (1, y), (1, 1 - y), (2, y), (3, y), (2, 1 - y), (3, 1 - y)]

    def pair_copy(array, turn):
        held = (gx, gc, pg, sq)[array]
        at, source = (unit_of(*turns[turn]), OTHER) if array < 2 else (PLACES[turn], OWN)
        return pltpu.make_async_remote_copy(
            src_ref=held.at[at, source], dst_ref=held.at[at, SIBLING],
            send_sem=pair_send.at[array, turn], recv_sem=pair_recv.at[array, turn],
            device_id=sibling, device_id_type=MESH,
        )

    def ready_same(index, turn):
        done = first if index == 0 else far_y if index == depth - 1 else []
        for sub in subs:
            if sub not in done:
                arrive(sub, (planes[index], y, 1 - tp))
        for array in range(2):
            pair_copy(array, turn).start()

    def ready_other(index, turn):
        done = second if index == 0 else far_x if index == depth - 1 else []
        for sub in subs:
            if sub not in done:
                arrive(sub, (planes[index], 1 - y, tp))
        if index == depth - 1:
            for sub in subs:
                arrive(sub, (last, 1 - y, 1 - tp), far)
        for array in range(2):
            pair_copy(array, turn).start()

    def compute(turn):
        unit, place = unit_of(*turns[turn]), PLACES[turn]
        tile = hidden // 4

        @pl.loop(0, hidden // tile)
        def _(step):
            cols = pl.ds(pl.multiple_of(step * tile, tile), tile)
            preact = (
                jnp.dot(gx[unit, OWN], up[0, :, cols], preferred_element_type=jnp.float32)
                + jnp.dot(gx[unit, OTHER], up[1, :, cols], preferred_element_type=jnp.float32)
            )
            act_grad = (
                jnp.dot(gc[unit, OWN], down[0, :, cols], preferred_element_type=jnp.float32)
                + jnp.dot(gc[unit, OTHER], down[1, :, cols], preferred_element_type=jnp.float32)
            )
            relu_pre = jnp.maximum(preact, 0.0)
            sq[place, OWN, :, cols] = (relu_pre * relu_pre).astype(sq.dtype)
            pg[place, OWN, :, cols] = (2.0 * relu_pre * act_grad).astype(pg.dtype)

        for array in (2, 3):
            pair_copy(array, turn).start()

    def both(ref, unit, cols):
        block = ref[unit, pl.ds(OWN, 2), :, cols]
        return block.reshape(2 * height, block.shape[2])

    def gather_pair(first_turn):
        for turn in (first_turn, first_turn + 1):
            for array in range(4):
                pair_copy(array, turn).wait_recv()

    def weight_grad(first_turn, into, left, right):
        rows, cols = into.shape
        span, tile = width, 256
        pair = (first_turn, first_turn + 1)

        def block(ref, turn, cols):
            return both(ref, unit_of(*turns[turn]) if ref is gx or ref is gc else PLACES[turn], cols)

        @pl.loop(0, (rows // span) * (cols // tile))
        def _(step):
            at = pl.ds(pl.multiple_of((step // (cols // tile)) * span, span), span)
            across = pl.ds(pl.multiple_of((step % (cols // tile)) * tile, tile), tile)
            total = sum(contract_rows(block(left, turn, at), block(right, turn, across)) for turn in pair)
            into[at, across] = total if first_turn == 0 else into[at, across] + total

    def partial():
        tile = width // 4

        @pl.loop(0, width // tile)
        def _(step):
            cols = pl.ds(pl.multiple_of(step * tile, tile), tile)
            for slot, into in (((tp + fs) % 2, mine), ((tp + fs + 1) % 2, sent)):
                into[:, cols] = contract_cols(pg[PLACES[0], OWN], up[slot, cols, :]).astype(into.dtype)

    part_copy = pltpu.make_async_remote_copy(
        src_ref=sent, dst_ref=theirs, send_sem=part_sem.at[0], recv_sem=part_sem.at[1],
        device_id=target[X], device_id_type=MESH,
    )
    swap_up = pltpu.make_async_remote_copy(
        src_ref=up_ref, dst_ref=up.at[1], send_sem=swap_sem.at[0], recv_sem=swap_sem.at[1],
        device_id=sibling, device_id_type=MESH,
    )

    def turn_copy(number):
        cols = pl.ds(number * chunk, chunk)
        return pltpu.make_async_remote_copy(
            src_ref=down.at[0, :, cols], dst_ref=down.at[1, :, cols],
            send_sem=turn_sem.at[0, number], recv_sem=turn_sem.at[1, number],
            device_id=sibling, device_id_type=MESH,
        )

    for own in owns:
        own.wait()
    here = (z, y, tp)
    for k, sub in enumerate(subs):
        start(UP, sub, here, above)
        start(DOWN, sub, here, below)
        start(X, sub, here)
        start(Y, (second + first)[k], here)
    swap_up.start()
    for number in range(chunks):
        stage_copy(number).wait()
        down[0, :, pl.ds(number * chunk, chunk)] = stage[number % 2].T
        if number + 2 < chunks:
            stage_copy(number + 2).start()
        turn_copy(number).start()

    cross(first[0], second[0])
    column(1, subs[0])
    cross(first[1], second[1])
    for sub in subs[1:]:
        column(1, sub)
    ready_same(0, 0)
    own_up.wait()
    swap_up.wait()
    for number in range(chunks):
        turn_copy(number).wait()
    compute(0)
    for sub in subs:
        corner_own(sub)
    for sub in subs[:2]:
        column(2, sub)
    ready_other(0, 1)
    compute(1)
    for sub in subs[2:]:
        column(2, sub)
    partial()
    gather_pair(0)
    weight_grad(0, acc_up, gx, pg)
    ready_same(1, 2)
    compute(2)
    weight_grad(0, acc_down, sq, gc)
    pl.semaphore_signal(free_sem, inc=1, device_id=sibling, device_id_type=MESH)
    for sub in subs:
        corner(1, sub)
    for sub in subs[:2]:
        column(3, sub)
    ready_other(1, 3)
    compute(3)
    for sub in subs[2:]:
        column(3, sub)
    for turn in (0, 1):
        for array in (2, 3):
            pair_copy(array, turn).wait_send()
    pl.semaphore_wait(free_sem, 1)
    gather_pair(2)
    weight_grad(2, acc_up, gx, pg)
    ready_same(2, 4)
    compute(4)
    for sub in subs:
        far_cross(sub)
    part_copy.start()
    weight_grad(2, acc_down, sq, gc)
    ready_same(3, 5)
    compute(5)
    for sub in subs:
        corner(2, sub)
    gather_pair(4)
    weight_grad(4, acc_up, gx, pg)
    ready_other(2, 6)
    compute(6)
    ready_other(3, 7)
    compute(7)
    weight_grad(4, acc_down, sq, gc)
    gather_pair(6)
    part_copy.wait()
    for way, sub, at, condition in started:
        if condition is None:
            copy(way, sub, at).wait_send()
        else:
            pl.when(condition)(functools.partial(lambda w, s, a: copy(w, s, a).wait_send(), way, sub, at))
    for turn in range(len(turns)):
        for array in range(4):
            if array < 2 or turn >= 2:
                pair_copy(array, turn).wait_send()


def finish_kernel(reps, acc_up, acc_down, gx, gc, pg, sq, mine, theirs,
                  inputs_out, up_out, down_out, tiles, added, tile_sem, added_sem):
    rep = lax.axis_index("rep")
    z, y = rep // PAIR, rep % PAIR
    depth = reps // PAIR
    units = [nearest(z, depth, index) * PAIR + (1 - y) for index in (depth - 2, depth - 1)]
    height = gx.shape[2]
    slots, span, tile = tiles.shape

    added[...] = (mine[...].astype(jnp.float32) + theirs[...].astype(jnp.float32)).astype(added.dtype)
    put = pltpu.make_async_copy(added, inputs_out, added_sem)
    put.start()

    def both(ref, unit, cols):
        block = ref[unit, pl.ds(OWN, 2), :, cols]
        return block.reshape(2 * height, block.shape[2])

    base = 0
    for held, out, left, right in ((acc_up, up_out, gx, pg), (acc_down, down_out, sq, gc)):
        rows, cols = held.shape
        across_count = cols // tile
        count = (rows // span) * across_count

        def place(step):
            return (
                pl.ds(pl.multiple_of((step // across_count) * span, span), span),
                pl.ds(pl.multiple_of((step % across_count) * tile, tile), tile),
            )

        def out_copy(step, slot):
            at, across = place(step)
            return pltpu.make_async_copy(tiles.at[slot], out.at[at, across], tile_sem.at[slot])

        @pl.loop(0, count)
        def _(step):
            slot = step % slots
            pl.when(step >= slots)(lambda: out_copy(step - slots, slot).wait())
            at, across = place(step)
            total = sum(
                contract_rows(both(left, one, at), both(right, other, across))
                for one, other in zip(*((units, PLACES[-2:]) if right is pg else (PLACES[-2:], units)))
            )
            tiles[slot] = held[at, across] + total
            out_copy(step, slot).start()

        for step in range(count - slots, count):
            out_copy(step, step % slots).wait()
    put.wait()


def few_tokens(reps, inputs, cotangent, w_up, w_down):
    height, width = inputs.shape
    hidden = w_up.shape[1]
    depth = reps // PAIR
    low, high = inputs.dtype, jnp.float32
    far, vmem = pl.BlockSpec(memory_space=pltpu.HBM), pl.BlockSpec(memory_space=pltpu.VMEM)
    blocks, rows = (reps, 3, height, width), (max(PLACES) + 1, 2, height, hidden)
    shapes = [(w_up.shape, high), (w_down.shape, high), (blocks, low), (blocks, low), (rows, low), (rows, low),
              (inputs.shape, low), (inputs.shape, low)]
    chunk = w_down.shape[0] // 8
    tokens = reps * height
    held = pl.pallas_call(
        functools.partial(hidden_kernel, reps),
        out_shape=[pltpu.VMEM(shape, dtype) for shape, dtype in shapes],
        in_specs=[far] * 4,
        out_specs=[vmem] * len(shapes),
        scratch_shapes=[
            pltpu.VMEM((2,) + w_up.shape, low),
            pltpu.VMEM((2, width, hidden), low),
            pltpu.VMEM((2, chunk, width), low),
            pltpu.VMEM(inputs.shape, low),
            pltpu.SemaphoreType.REGULAR,
            pltpu.SemaphoreType.DMA((4, 4, reps * 2)),
            pltpu.SemaphoreType.DMA((4, reps * 2)),
            pltpu.SemaphoreType.DMA((2,)),
            pltpu.SemaphoreType.DMA((2, 8)),
            pltpu.SemaphoreType.DMA((3,)),
            pltpu.SemaphoreType.DMA((2,)),
            pltpu.SemaphoreType.DMA((4, reps)),
            pltpu.SemaphoreType.DMA((4, reps)),
            pltpu.SemaphoreType.DMA((2,)),
        ],
        cost_estimate=pl.CostEstimate(flops=14 * tokens * width * hidden, bytes_accessed=w_up.size * 8, transcendentals=0),
        compiler_params=pltpu.CompilerParams(
            collective_id=0, has_side_effects=True, vmem_limit_bytes=GRANT
        ),
    )(*(pltpu.with_memory_space_constraint(value, pltpu.HBM) for value in (inputs, cotangent, w_up, w_down)))
    return pl.pallas_call(
        functools.partial(finish_kernel, reps),
        out_shape=[
            jax.ShapeDtypeStruct(inputs.shape, low),
            jax.ShapeDtypeStruct(w_up.shape, high),
            jax.ShapeDtypeStruct(w_down.shape, high),
        ],
        in_specs=[vmem] * len(shapes),
        out_specs=[far] * 3,
        scratch_shapes=[
            pltpu.VMEM((4, width, 256), high),
            pltpu.VMEM(inputs.shape, low),
            pltpu.SemaphoreType.DMA((4,)),
            pltpu.SemaphoreType.DMA,
        ],
        cost_estimate=pl.CostEstimate(flops=16 * height * width * hidden, bytes_accessed=w_up.size * 16, transcendentals=0),
        compiler_params=pltpu.CompilerParams(vmem_limit_bytes=GRANT),
    )(*(pltpu.with_memory_space_constraint(value, pltpu.VMEM) for value in held))


def many_tokens(inputs, cotangent, w_up, w_down):
    rows_in, rows_cot = (
        lax.all_gather(inputs, "tp", axis=1, tiled=True),
        lax.all_gather(cotangent, "tp", axis=1, tiled=True),
    )
    cols_in, cols_cot = (
        lax.all_to_all(rows_in, "fs", split_axis=1, concat_axis=0, tiled=True),
        lax.all_to_all(rows_cot, "fs", split_axis=1, concat_axis=0, tiled=True),
    )
    full_up, full_down = (
        lax.all_gather(w_up, "fs", axis=0, tiled=True),
        lax.all_gather(w_down, "fs", axis=1, tiled=True),
    )
    act_grad = contract_cols(rows_cot, full_down)
    preact = jnp.dot(rows_in, full_up, preferred_element_type=jnp.float32)
    relu_pre = jnp.maximum(preact, 0.0)
    squared = (relu_pre * relu_pre).astype(jnp.bfloat16)
    pre_grad = (2.0 * relu_pre * act_grad).astype(jnp.bfloat16)
    partial_value = contract_cols(pre_grad, full_up)
    grad_inputs = lax.psum_scatter(
        partial_value.astype(jnp.bfloat16), "tp", scatter_dimension=1, tiled=True
    )
    grad_piece = lax.all_gather(pre_grad, "fs", axis=0, tiled=True)
    square_piece = lax.all_gather(squared, "fs", axis=0, tiled=True)
    local_up = contract_rows(cols_in, grad_piece)
    local_down = contract_rows(square_piece, cols_cot)
    slice_up = lax.psum_scatter(local_up, "rep", scatter_dimension=0, tiled=True)
    slice_down = lax.psum_scatter(local_down, "rep", scatter_dimension=0, tiled=True)
    grad_up = lax.all_gather(slice_up, "rep", axis=0, tiled=True)
    grad_down = lax.all_gather(slice_down, "rep", axis=0, tiled=True)
    return (grad_inputs, grad_up, grad_down)


def solution(mesh):
    reps, n_fs, n_tp = mesh.shape["rep"], mesh.shape["fs"], mesh.shape["tp"]

    def shards(inputs, cotangent, w_up, w_down):
        gathered = 2 * reps * n_tp * inputs.size * inputs.dtype.itemsize
        gradients = (w_up.size + w_down.size) * 4
        fits = n_fs == 2 and n_tp == 2 and reps == PAIR * 4 and inputs.shape[0] % 32 == 0
        if fits and gathered <= gradients:
            return few_tokens(reps, inputs, cotangent, w_up, w_down)
        return many_tokens(inputs, cotangent, w_up, w_down)

    return jax.shard_map(
        shards,
        mesh=mesh,
        in_specs=(P(("rep", "fs"), "tp"), P(("rep", "fs"), "tp"), P("fs", "tp"), P("tp", "fs")),
        out_specs=(P(("rep", "fs"), "tp"), P("fs", "tp"), P("tp", "fs")),
        check_vma=False,
    )
```

```python
import functools

import jax
import jax.numpy as jnp
from jax import lax
from jax.experimental import pallas as pl
from jax.experimental.pallas import tpu as pltpu
from jax.sharding import PartitionSpec as P

MESH = pl.DeviceIdType.MESH
X, Y, UP, DOWN = range(4)
PAIR = 2
OWN, SIBLING, OTHER = range(3)
PLACES = (0, 1, 2, 3, 0, 1, 4, 5)
GRANT = 22 * 1024 * 1024


def contract_rows(left, right):
    return lax.dot_general(
        left, right, (((0,), (0,)), ((), ())), preferred_element_type=jnp.float32
    )


def contract_cols(left, right):
    return lax.dot_general(
        left, right, (((1,), (1,)), ((), ())), preferred_element_type=jnp.float32
    )


def nearest(z, depth, index):
    near = jnp.minimum(z, depth - 1 - z)
    away = (index + 1) // 2
    around = z - away if index % 2 else z + away
    outward = jnp.where(z < depth - 1 - z, z + (index - near), z - (index - near))
    return jnp.where(index <= 2 * near, around, outward)


def hidden_kernel(reps, x_ref, c_ref, up_ref, down_ref,
                  acc_up, acc_down, gx, gc, pg, sq, mine, theirs,
                  up, down, stage, sent,
                  free_sem, send_sem, recv_sem, swap_sem, turn_sem, own_sem, stage_sem,
                  pair_send, pair_recv, part_sem):
    rep, fs, tp = lax.axis_index("rep"), lax.axis_index("fs"), lax.axis_index("tp")
    z, y = rep // PAIR, rep % PAIR
    depth = reps // PAIR
    height, width = x_ref.shape
    half = height // 2
    hidden = up.shape[2]
    reach = depth - 2
    target = {
        X: {"tp": 1 - tp},
        Y: {"rep": z * PAIR + (1 - y)},
        UP: {"rep": jnp.minimum(z + 1, depth - 1) * PAIR + y},
        DOWN: {"rep": jnp.maximum(z - 1, 0) * PAIR + y},
    }
    sibling = {"fs": 1 - fs}
    above, below = z < depth - 1, z > 0
    planes = [nearest(z, depth, index) for index in range(depth)]
    own_block = ((tp + fs) % 2) * OTHER

    chunk = stage.shape[1]
    chunks = down_ref.shape[0] // chunk

    def stage_copy(number):
        rows = pl.ds(number * chunk, chunk)
        return pltpu.make_async_copy(down_ref.at[rows], stage.at[number % 2], stage_sem.at[number % 2])

    owns = [
        pltpu.make_async_copy(x_ref, gx.at[rep, own_block], own_sem.at[0]),
        pltpu.make_async_copy(c_ref, gc.at[rep, own_block], own_sem.at[1]),
    ]
    for own in owns:
        own.start()
    stage_copy(0).start()
    stage_copy(1).start()
    own_up = pltpu.make_async_copy(up_ref, up.at[0], own_sem.at[2])
    own_up.start()

    barrier = pltpu.get_barrier_semaphore()

    def greet(device):
        pl.semaphore_signal(barrier, inc=1, device_id=device, device_id_type=MESH)

    greet(target[X])
    greet(target[Y])
    greet(sibling)
    pl.when(above)(lambda: greet(target[UP]))
    pl.when(below)(lambda: greet(target[DOWN]))
    pl.semaphore_wait(barrier, 3 + above.astype(jnp.int32) + below.astype(jnp.int32))

    started = []

    def copy(way, sub, at):
        at_z, at_y, at_t = at
        array, part = sub
        unit = at_z * PAIR + at_y
        place = (gx, gc)[array].at[unit, ((at_t + fs) % 2) * OTHER, pl.ds(part * half, half)]
        index, piece = array * 2 + part, unit * 2 + at_t
        return pltpu.make_async_remote_copy(
            src_ref=place, dst_ref=place,
            send_sem=send_sem.at[way, index, piece], recv_sem=recv_sem.at[index, piece],
            device_id=target[way], device_id_type=MESH,
        )

    def start(way, sub, at, condition=None):
        if condition is None:
            copy(way, sub, at).start()
        else:
            pl.when(condition)(lambda: copy(way, sub, at).start())
        started.append((way, sub, at, condition))

    def arrive(sub, at, condition=None):
        if condition is None:
            copy(X, sub, at).wait_recv()
        else:
            pl.when(condition)(lambda: copy(X, sub, at).wait_recv())

    first = [(array, 0) for array in range(2)]
    second = [(array, 1) for array in range(2)]
    subs = first + second
    far_y, far_x = subs[:3], subs[3:]

    def sides(distance):
        return (
            (z - distance, z >= distance, UP, jnp.logical_and(z >= distance, above)),
            (z + distance, z + distance < depth, DOWN, jnp.logical_and(z + distance < depth, below)),
        )

    def column(distance, sub):
        for at_z, there, way, onward in sides(distance):
            at = (at_z, y, tp)
            arrive(sub, at, there)
            start(way, sub, at, onward)
            start(X, sub, at, there)
            start(Y, sub, at, there)

    def cross(one, two):
        arrive(one, (z, y, 1 - tp))
        start(Y, one, (z, y, 1 - tp))
        arrive(two, (z, 1 - y, tp))
        start(X, two, (z, 1 - y, tp))

    def corner_own(sub):
        at = (z, 1 - y, 1 - tp)
        arrive(sub, at)
        start(UP, sub, at, above)
        start(DOWN, sub, at, below)

    def corner(distance, sub):
        for at_z, there, way, onward in sides(distance):
            at = (at_z, 1 - y, 1 - tp)
            arrive(sub, at, there)
            if distance < reach:
                start(way, sub, at, onward)

    last = planes[depth - 1]
    far = jnp.logical_or(last - z > reach, z - last > reach)

    def far_cross(sub):
        if sub in far_y:
            arrive(sub, (last, y, 1 - tp))
            start(Y, sub, (last, y, 1 - tp), far)
        else:
            arrive(sub, (last, 1 - y, tp))
            start(X, sub, (last, 1 - y, tp), far)

    def unit_of(index, row):
        return planes[index] * PAIR + row

    turns = [(0, y), (0, 1 - y), (1, y), (1, 1 - y), (2, y), (3, y), (2, 1 - y), (3, 1 - y)]

    def pair_copy(array, turn):
        held = (gx, gc, pg, sq)[array]
        at, source = (unit_of(*turns[turn]), OTHER) if array < 2 else (PLACES[turn], OWN)
        return pltpu.make_async_remote_copy(
            src_ref=held.at[at, source], dst_ref=held.at[at, SIBLING],
            send_sem=pair_send.at[array, turn], recv_sem=pair_recv.at[array, turn],
            device_id=sibling, device_id_type=MESH,
        )

    def ready_same(index, turn):
        done = first if index == 0 else far_y if index == depth - 1 else []
        for sub in subs:
            if sub not in done:
                arrive(sub, (planes[index], y, 1 - tp))
        for array in range(2):
            pair_copy(array, turn).start()

    def ready_other(index, turn):
        done = second if index == 0 else far_x if index == depth - 1 else []
        for sub in subs:
            if sub not in done:
                arrive(sub, (planes[index], 1 - y, tp))
        if index == depth - 1:
            for sub in subs:
                arrive(sub, (last, 1 - y, 1 - tp), far)
        for array in range(2):
            pair_copy(array, turn).start()

    def compute(turn, lo=0, hi=2):
        unit, place = unit_of(*turns[turn]), PLACES[turn]
        tile = hidden // 2

        @pl.loop(lo, hi)
        def _(step):
            cols = pl.ds(pl.multiple_of(step * tile, tile), tile)
            preact = (
                jnp.dot(gx[unit, OWN], up[0, :, cols], preferred_element_type=jnp.float32)
                + jnp.dot(gx[unit, OTHER], up[1, :, cols], preferred_element_type=jnp.float32)
            )
            act_grad = (
                jnp.dot(gc[unit, OWN], down[0, :, cols], preferred_element_type=jnp.float32)
                + jnp.dot(gc[unit, OTHER], down[1, :, cols], preferred_element_type=jnp.float32)
            )
            relu_pre = jnp.maximum(preact, 0.0)
            sq[place, OWN, :, cols] = (relu_pre * relu_pre).astype(sq.dtype)
            pg[place, OWN, :, cols] = (2.0 * relu_pre * act_grad).astype(pg.dtype)

        if hi == 2:
            for array in (2, 3):
                pair_copy(array, turn).start()

    def both(ref, unit, cols):
        block = ref[unit, pl.ds(OWN, 2), :, cols]
        return block.reshape(2 * height, block.shape[2])

    def gather_pair(first_turn):
        for turn in (first_turn, first_turn + 1):
            for array in range(4):
                pair_copy(array, turn).wait_recv()

    def weight_grad(first_turn, into, left, right, lo=0, hi=None, parts=1):
        rows, cols = into.shape
        span, tile = width // parts, 256
        pair = (first_turn, first_turn + 1)

        def block(ref, turn, cols):
            return both(ref, unit_of(*turns[turn]) if ref is gx or ref is gc else PLACES[turn], cols)

        @pl.loop(lo, rows // span if hi is None else hi)
        def _(step):
            at = pl.ds(pl.multiple_of(step * span, span), span)
            lefts = [block(left, turn, at) for turn in pair]
            for number in range(cols // tile):
                across = pl.ds(number * tile, tile)
                total = sum(contract_rows(one, block(right, turn, across)) for one, turn in zip(lefts, pair))
                into[at, across] = total if first_turn == 0 else into[at, across] + total

    def partial():
        tile = width // 4

        @pl.loop(0, width // tile)
        def _(step):
            cols = pl.ds(pl.multiple_of(step * tile, tile), tile)
            for slot, into in (((tp + fs) % 2, mine), ((tp + fs + 1) % 2, sent)):
                into[:, cols] = contract_cols(pg[PLACES[0], OWN], up[slot, cols, :]).astype(into.dtype)

    part_copy = pltpu.make_async_remote_copy(
        src_ref=sent, dst_ref=theirs, send_sem=part_sem.at[0], recv_sem=part_sem.at[1],
        device_id=target[X], device_id_type=MESH,
    )
    swap_up = pltpu.make_async_remote_copy(
        src_ref=up_ref, dst_ref=up.at[1], send_sem=swap_sem.at[0], recv_sem=swap_sem.at[1],
        device_id=sibling, device_id_type=MESH,
    )

    def turn_copy(number):
        cols = pl.ds(number * chunk, chunk)
        return pltpu.make_async_remote_copy(
            src_ref=down.at[0, :, cols], dst_ref=down.at[1, :, cols],
            send_sem=turn_sem.at[0, number], recv_sem=turn_sem.at[1, number],
            device_id=sibling, device_id_type=MESH,
        )

    for own in owns:
        own.wait()
    here = (z, y, tp)
    for k, sub in enumerate(subs):
        start(UP, sub, here, above)
        start(DOWN, sub, here, below)
        start(X, sub, here)
        start(Y, (second + first)[k], here)
    swap_up.start()
    for number in range(chunks):
        stage_copy(number).wait()
        down[0, :, pl.ds(number * chunk, chunk)] = stage[number % 2].T
        if number + 2 < chunks:
            stage_copy(number + 2).start()
        turn_copy(number).start()

    cross(first[0], second[0])
    column(1, subs[0])
    cross(first[1], second[1])
    for sub in subs[1:]:
        column(1, sub)
    ready_same(0, 0)
    own_up.wait()
    swap_up.wait()
    for number in range(chunks):
        turn_copy(number).wait()
    compute(0)
    for sub in subs:
        corner_own(sub)
    for sub in subs[:2]:
        column(2, sub)
    ready_other(0, 1)
    compute(1)
    for sub in subs[2:]:
        column(2, sub)
    partial()
    gather_pair(0)
    weight_grad(0, acc_up, gx, pg)
    weight_grad(0, acc_down, sq, gc, 0, 1)
    ready_same(1, 2)
    compute(2)
    weight_grad(0, acc_down, sq, gc, 1, 2)
    pl.semaphore_signal(free_sem, inc=1, device_id=sibling, device_id_type=MESH)
    for sub in subs:
        corner(1, sub)
    ready_other(1, 3)
    compute(3)
    for sub in subs[:2]:
        column(3, sub)
    for turn in (0, 1):
        for array in (2, 3):
            pair_copy(array, turn).wait_send()
    pl.semaphore_wait(free_sem, 1)
    gather_pair(2)
    weight_grad(2, acc_up, gx, pg, 0, 1, 2)
    column(3, subs[2])
    ready_same(2, 4)
    compute(4, 0, 1)
    column(3, subs[3])
    compute(4, 1, 2)
    far_cross(subs[0])
    far_cross(subs[1])
    weight_grad(2, acc_up, gx, pg, 1, 2, 2)
    far_cross(subs[2])
    weight_grad(2, acc_down, sq, gc, 0, 1)
    far_cross(subs[3])
    part_copy.start()
    weight_grad(2, acc_down, sq, gc, 1, 2)
    ready_same(3, 5)
    compute(5)
    gather_pair(4)
    weight_grad(4, acc_up, gx, pg)
    for sub in subs:
        corner(2, sub)
    ready_other(2, 6)
    compute(6)
    ready_other(3, 7)
    compute(7)
    weight_grad(4, acc_down, sq, gc)
    gather_pair(6)
    part_copy.wait()
    for way, sub, at, condition in started:
        if condition is None:
            copy(way, sub, at).wait_send()
        else:
            pl.when(condition)(functools.partial(lambda w, s, a: copy(w, s, a).wait_send(), way, sub, at))
    for turn in range(len(turns)):
        for array in range(4):
            if array < 2 or turn >= 2:
                pair_copy(array, turn).wait_send()


def finish_kernel(reps, acc_up, acc_down, gx, gc, pg, sq, mine, theirs,
                  inputs_out, up_out, down_out, tiles, added, tile_sem, added_sem):
    rep = lax.axis_index("rep")
    z, y = rep // PAIR, rep % PAIR
    depth = reps // PAIR
    units = [nearest(z, depth, index) * PAIR + (1 - y) for index in (depth - 2, depth - 1)]
    height = gx.shape[2]
    slots, span, wide = tiles.shape
    tile = 256

    added[...] = (mine[...].astype(jnp.float32) + theirs[...].astype(jnp.float32)).astype(added.dtype)
    put = pltpu.make_async_copy(added, inputs_out, added_sem)
    put.start()

    def both(ref, unit, cols):
        block = ref[unit, pl.ds(OWN, 2), :, cols]
        return block.reshape(2 * height, block.shape[2])

    started = []
    for held, out, left, right in ((acc_up, up_out, gx, pg), (acc_down, down_out, sq, gc)):
        rows, cols = held.shape
        pairs = list(zip(*((units, PLACES[-2:]) if right is pg else (PLACES[-2:], units))))
        for at in (pl.ds(start, span) for start in range(0, rows, span)):
            lefts = [both(left, one, at) for one, _ in pairs]
            for begin in range(0, cols, wide):
                slot = len(started) % slots
                if len(started) >= slots:
                    started[-slots].wait()
                for start in range(0, wide, tile):
                    across = pl.ds(begin + start, tile)
                    total = sum(contract_rows(one, both(right, other, across)) for one, (_, other) in zip(lefts, pairs))
                    tiles[slot, :, pl.ds(start, tile)] = held[at, across] + total
                started.append(pltpu.make_async_copy(tiles.at[slot], out.at[at, pl.ds(begin, wide)], tile_sem.at[slot]))
                started[-1].start()
    for moved in started[-slots:]:
        moved.wait()
    put.wait()


def few_tokens(reps, inputs, cotangent, w_up, w_down):
    height, width = inputs.shape
    hidden = w_up.shape[1]
    depth = reps // PAIR
    low, high = inputs.dtype, jnp.float32
    far, vmem = pl.BlockSpec(memory_space=pltpu.HBM), pl.BlockSpec(memory_space=pltpu.VMEM)
    blocks, rows = (reps, 3, height, width), (max(PLACES) + 1, 2, height, hidden)
    shapes = [(w_up.shape, high), (w_down.shape, high), (blocks, low), (blocks, low), (rows, low), (rows, low),
              (inputs.shape, low), (inputs.shape, low)]
    chunk = w_down.shape[0] // 8
    tokens = reps * height
    held = pl.pallas_call(
        functools.partial(hidden_kernel, reps),
        out_shape=[pltpu.VMEM(shape, dtype) for shape, dtype in shapes],
        in_specs=[far] * 4,
        out_specs=[vmem] * len(shapes),
        scratch_shapes=[
            pltpu.VMEM((2,) + w_up.shape, low),
            pltpu.VMEM((2, width, hidden), low),
            pltpu.VMEM((2, chunk, width), low),
            pltpu.VMEM(inputs.shape, low),
            pltpu.SemaphoreType.REGULAR,
            pltpu.SemaphoreType.DMA((4, 4, reps * 2)),
            pltpu.SemaphoreType.DMA((4, reps * 2)),
            pltpu.SemaphoreType.DMA((2,)),
            pltpu.SemaphoreType.DMA((2, 8)),
            pltpu.SemaphoreType.DMA((3,)),
            pltpu.SemaphoreType.DMA((2,)),
            pltpu.SemaphoreType.DMA((4, reps)),
            pltpu.SemaphoreType.DMA((4, reps)),
            pltpu.SemaphoreType.DMA((2,)),
        ],
        cost_estimate=pl.CostEstimate(flops=14 * tokens * width * hidden, bytes_accessed=w_up.size * 8, transcendentals=0),
        compiler_params=pltpu.CompilerParams(
            collective_id=0, has_side_effects=True, vmem_limit_bytes=GRANT
        ),
    )(*(pltpu.with_memory_space_constraint(value, pltpu.HBM) for value in (inputs, cotangent, w_up, w_down)))
    return pl.pallas_call(
        functools.partial(finish_kernel, reps),
        out_shape=[
            jax.ShapeDtypeStruct(inputs.shape, low),
            jax.ShapeDtypeStruct(w_up.shape, high),
            jax.ShapeDtypeStruct(w_down.shape, high),
        ],
        in_specs=[vmem] * len(shapes),
        out_specs=[far] * 3,
        scratch_shapes=[
            pltpu.VMEM((4, width, width // 2), high),
            pltpu.VMEM(inputs.shape, low),
            pltpu.SemaphoreType.DMA((4,)),
            pltpu.SemaphoreType.DMA,
        ],
        cost_estimate=pl.CostEstimate(flops=16 * height * width * hidden, bytes_accessed=w_up.size * 16, transcendentals=0),
        compiler_params=pltpu.CompilerParams(vmem_limit_bytes=GRANT),
    )(*(pltpu.with_memory_space_constraint(value, pltpu.VMEM) for value in held))


def many_tokens(inputs, cotangent, w_up, w_down):
    rows_in, rows_cot = (
        lax.all_gather(inputs, "tp", axis=1, tiled=True),
        lax.all_gather(cotangent, "tp", axis=1, tiled=True),
    )
    cols_in, cols_cot = (
        lax.all_to_all(rows_in, "fs", split_axis=1, concat_axis=0, tiled=True),
        lax.all_to_all(rows_cot, "fs", split_axis=1, concat_axis=0, tiled=True),
    )
    full_up, full_down = (
        lax.all_gather(w_up, "fs", axis=0, tiled=True),
        lax.all_gather(w_down, "fs", axis=1, tiled=True),
    )
    act_grad = contract_cols(rows_cot, full_down)
    preact = jnp.dot(rows_in, full_up, preferred_element_type=jnp.float32)
    relu_pre = jnp.maximum(preact, 0.0)
    squared = (relu_pre * relu_pre).astype(jnp.bfloat16)
    pre_grad = (2.0 * relu_pre * act_grad).astype(jnp.bfloat16)
    partial_value = contract_cols(pre_grad, full_up)
    grad_inputs = lax.psum_scatter(
        partial_value.astype(jnp.bfloat16), "tp", scatter_dimension=1, tiled=True
    )
    grad_piece = lax.all_gather(pre_grad, "fs", axis=0, tiled=True)
    square_piece = lax.all_gather(squared, "fs", axis=0, tiled=True)
    local_up = contract_rows(cols_in, grad_piece)
    local_down = contract_rows(square_piece, cols_cot)
    slice_up = lax.psum_scatter(local_up, "rep", scatter_dimension=0, tiled=True)
    slice_down = lax.psum_scatter(local_down, "rep", scatter_dimension=0, tiled=True)
    grad_up = lax.all_gather(slice_up, "rep", axis=0, tiled=True)
    grad_down = lax.all_gather(slice_down, "rep", axis=0, tiled=True)
    return (grad_inputs, grad_up, grad_down)


def solution(mesh):
    reps, n_fs, n_tp = mesh.shape["rep"], mesh.shape["fs"], mesh.shape["tp"]

    def shards(inputs, cotangent, w_up, w_down):
        gathered = 2 * reps * n_tp * inputs.size * inputs.dtype.itemsize
        gradients = (w_up.size + w_down.size) * 4
        fits = n_fs == 2 and n_tp == 2 and reps == PAIR * 4 and inputs.shape[0] % 32 == 0
        if fits and gathered <= gradients:
            return few_tokens(reps, inputs, cotangent, w_up, w_down)
        return many_tokens(inputs, cotangent, w_up, w_down)

    return jax.shard_map(
        shards,
        mesh=mesh,
        in_specs=(P(("rep", "fs"), "tp"), P(("rep", "fs"), "tp"), P("fs", "tp"), P("tp", "fs")),
        out_specs=(P(("rep", "fs"), "tp"), P("fs", "tp"), P("tp", "fs")),
        check_vma=False,
    )
```

```python
import functools

import jax
import jax.numpy as jnp
from jax import lax
from jax.experimental import pallas as pl
from jax.experimental.pallas import tpu as pltpu
from jax.sharding import PartitionSpec as P

MESH = pl.DeviceIdType.MESH
X, Y, UP, DOWN = range(4)
PAIR = 2
OWN, SIBLING, OTHER = range(3)
PLACES = (0, 1, 2, 3, 0, 1, 4, 5)
GRANT = 22 * 1024 * 1024


def contract_rows(left, right):
    return lax.dot_general(
        left, right, (((0,), (0,)), ((), ())), preferred_element_type=jnp.float32
    )


def contract_cols(left, right):
    return lax.dot_general(
        left, right, (((1,), (1,)), ((), ())), preferred_element_type=jnp.float32
    )


def nearest(z, depth, index):
    near = jnp.minimum(z, depth - 1 - z)
    away = (index + 1) // 2
    around = z - away if index % 2 else z + away
    outward = jnp.where(z < depth - 1 - z, z + (index - near), z - (index - near))
    return jnp.where(index <= 2 * near, around, outward)


def hidden_kernel(reps, x_ref, c_ref, up_ref, down_ref,
                  acc_up, acc_down, gx, gc, pg, sq, mine, theirs,
                  up, down, stage, sent,
                  free_sem, send_sem, recv_sem, swap_sem, turn_sem, own_sem, stage_sem,
                  pair_send, pair_recv, part_sem):
    rep, fs, tp = lax.axis_index("rep"), lax.axis_index("fs"), lax.axis_index("tp")
    z, y = rep // PAIR, rep % PAIR
    depth = reps // PAIR
    height, width = x_ref.shape
    half = height // 2
    hidden = up.shape[2]
    reach = depth - 2
    target = {
        X: {"tp": 1 - tp},
        Y: {"rep": z * PAIR + (1 - y)},
        UP: {"rep": jnp.minimum(z + 1, depth - 1) * PAIR + y},
        DOWN: {"rep": jnp.maximum(z - 1, 0) * PAIR + y},
    }
    sibling = {"fs": 1 - fs}
    above, below = z < depth - 1, z > 0
    planes = [nearest(z, depth, index) for index in range(depth)]
    own_block = ((tp + fs) % 2) * OTHER

    chunk = stage.shape[1]
    chunks = down_ref.shape[0] // chunk

    def stage_copy(number):
        rows = pl.ds(number * chunk, chunk)
        return pltpu.make_async_copy(down_ref.at[rows], stage.at[number % 2], stage_sem.at[number % 2])

    owns = [
        pltpu.make_async_copy(x_ref, gx.at[rep, own_block], own_sem.at[0]),
        pltpu.make_async_copy(c_ref, gc.at[rep, own_block], own_sem.at[1]),
    ]
    for own in owns:
        own.start()
    stage_copy(0).start()
    stage_copy(1).start()
    own_up = pltpu.make_async_copy(up_ref, up.at[0], own_sem.at[2])
    own_up.start()

    barrier = pltpu.get_barrier_semaphore()

    def greet(device):
        pl.semaphore_signal(barrier, inc=1, device_id=device, device_id_type=MESH)

    greet(target[X])
    greet(target[Y])
    greet(sibling)
    pl.when(above)(lambda: greet(target[UP]))
    pl.when(below)(lambda: greet(target[DOWN]))
    pl.semaphore_wait(barrier, 3 + above.astype(jnp.int32) + below.astype(jnp.int32))

    started = []

    def copy(way, sub, at):
        at_z, at_y, at_t = at
        array, part = sub
        unit = at_z * PAIR + at_y
        place = (gx, gc)[array].at[unit, ((at_t + fs) % 2) * OTHER, pl.ds(part * half, half)]
        index, piece = array * 2 + part, unit * 2 + at_t
        return pltpu.make_async_remote_copy(
            src_ref=place, dst_ref=place,
            send_sem=send_sem.at[way, index, piece], recv_sem=recv_sem.at[index, piece],
            device_id=target[way], device_id_type=MESH,
        )

    def start(way, sub, at, condition=None):
        if condition is None:
            copy(way, sub, at).start()
        else:
            pl.when(condition)(lambda: copy(way, sub, at).start())
        started.append((way, sub, at, condition))

    def arrive(sub, at, condition=None):
        if condition is None:
            copy(X, sub, at).wait_recv()
        else:
            pl.when(condition)(lambda: copy(X, sub, at).wait_recv())

    first = [(array, 0) for array in range(2)]
    second = [(array, 1) for array in range(2)]
    subs = first + second
    far_y, far_x = first, second

    def sides(distance):
        return (
            (z - distance, z >= distance, UP, jnp.logical_and(z >= distance, above)),
            (z + distance, z + distance < depth, DOWN, jnp.logical_and(z + distance < depth, below)),
        )

    def spread(sub, side):
        at_z, there, _, _ = side
        start(X, sub, (at_z, y, tp), there)
        start(Y, sub, (at_z, y, tp), there)

    def column(distance, sub, defer=False):
        for side in sides(distance):
            at_z, there, way, onward = side
            arrive(sub, (at_z, y, tp), there)
            start(way, sub, (at_z, y, tp), onward)
            if way == UP or not defer:
                spread(sub, side)

    def cross(one, two):
        arrive(one, (z, y, 1 - tp))
        start(Y, one, (z, y, 1 - tp))
        arrive(two, (z, 1 - y, tp))
        start(X, two, (z, 1 - y, tp))

    def corner_own(sub):
        at = (z, 1 - y, 1 - tp)
        arrive(sub, at)
        start(UP, sub, at, above)
        start(DOWN, sub, at, below)

    def corner(distance, sub):
        for at_z, there, way, onward in sides(distance):
            at = (at_z, 1 - y, 1 - tp)
            arrive(sub, at, there)
            if distance < reach:
                start(way, sub, at, onward)

    last = planes[depth - 1]
    far = jnp.logical_or(last - z > reach, z - last > reach)

    def far_cross(sub):
        if sub in far_y:
            arrive(sub, (last, y, 1 - tp))
            start(Y, sub, (last, y, 1 - tp), far)
        else:
            arrive(sub, (last, 1 - y, tp))
            start(X, sub, (last, 1 - y, tp), far)

    def unit_of(index, row):
        return planes[index] * PAIR + row

    turns = [(0, y), (0, 1 - y), (1, y), (1, 1 - y), (2, y), (3, y), (2, 1 - y), (3, 1 - y)]

    def pair_copy(array, turn):
        held = (gx, gc, pg, sq)[array]
        at, source = (unit_of(*turns[turn]), OTHER) if array < 2 else (PLACES[turn], OWN)
        return pltpu.make_async_remote_copy(
            src_ref=held.at[at, source], dst_ref=held.at[at, SIBLING],
            send_sem=pair_send.at[array, turn], recv_sem=pair_recv.at[array, turn],
            device_id=sibling, device_id_type=MESH,
        )

    def ready_same(index, turn):
        done = first if index == 0 else far_y if index == depth - 1 else []
        for sub in subs:
            if sub not in done:
                arrive(sub, (planes[index], y, 1 - tp))
        for array in range(2):
            pair_copy(array, turn).start()

    def ready_other(index, turn):
        done = second if index == 0 else far_x if index == depth - 1 else []
        for sub in subs:
            if sub not in done:
                arrive(sub, (planes[index], 1 - y, tp))
        if index == depth - 1:
            for sub in subs:
                arrive(sub, (last, 1 - y, 1 - tp), far)
        for array in range(2):
            pair_copy(array, turn).start()

    def compute(turn, lo=0, hi=2):
        unit, place = unit_of(*turns[turn]), PLACES[turn]
        tile = hidden // 2

        @pl.loop(lo, hi)
        def _(step):
            cols = pl.ds(pl.multiple_of(step * tile, tile), tile)
            preact = (
                jnp.dot(gx[unit, OWN], up[0, :, cols], preferred_element_type=jnp.float32)
                + jnp.dot(gx[unit, OTHER], up[1, :, cols], preferred_element_type=jnp.float32)
            )
            act_grad = (
                jnp.dot(gc[unit, OWN], down[0, :, cols], preferred_element_type=jnp.float32)
                + jnp.dot(gc[unit, OTHER], down[1, :, cols], preferred_element_type=jnp.float32)
            )
            relu_pre = jnp.maximum(preact, 0.0)
            sq[place, OWN, :, cols] = (relu_pre * relu_pre).astype(sq.dtype)
            pg[place, OWN, :, cols] = (2.0 * relu_pre * act_grad).astype(pg.dtype)

        if hi == 2:
            for array in (2, 3):
                pair_copy(array, turn).start()

    def both(ref, unit, cols):
        block = ref[unit, pl.ds(OWN, 2), :, cols]
        return block.reshape(2 * height, block.shape[2])

    def gather(*several):
        for turn in several:
            for array in range(4):
                pair_copy(array, turn).wait_recv()

    def weight_grad(several, into, left, right, lo=0, hi=None, parts=1):
        rows, cols = into.shape
        span, tile = width // parts, 256

        def block(ref, turn, cols):
            return both(ref, unit_of(*turns[turn]) if ref is gx or ref is gc else PLACES[turn], cols)

        @pl.loop(lo, rows // span if hi is None else hi)
        def _(step):
            at = pl.ds(pl.multiple_of(step * span, span), span)
            lefts = [block(left, turn, at) for turn in several]
            for number in range(cols // tile):
                across = pl.ds(number * tile, tile)
                total = sum(contract_rows(one, block(right, turn, across)) for one, turn in zip(lefts, several))
                into[at, across] = total if 0 in several else into[at, across] + total

    def partial():
        tile = width // 4

        @pl.loop(0, width // tile)
        def _(step):
            cols = pl.ds(pl.multiple_of(step * tile, tile), tile)
            for slot, into in (((tp + fs) % 2, mine), ((tp + fs + 1) % 2, sent)):
                into[:, cols] = contract_cols(pg[PLACES[0], OWN], up[slot, cols, :]).astype(into.dtype)

    part_copy = pltpu.make_async_remote_copy(
        src_ref=sent, dst_ref=theirs, send_sem=part_sem.at[0], recv_sem=part_sem.at[1],
        device_id=target[X], device_id_type=MESH,
    )
    swap_up = pltpu.make_async_remote_copy(
        src_ref=up_ref, dst_ref=up.at[1], send_sem=swap_sem.at[0], recv_sem=swap_sem.at[1],
        device_id=sibling, device_id_type=MESH,
    )

    def turn_copy(number):
        cols = pl.ds(number * chunk, chunk)
        return pltpu.make_async_remote_copy(
            src_ref=down.at[0, :, cols], dst_ref=down.at[1, :, cols],
            send_sem=turn_sem.at[0, number], recv_sem=turn_sem.at[1, number],
            device_id=sibling, device_id_type=MESH,
        )

    for own in owns:
        own.wait()
    here = (z, y, tp)
    for k, sub in enumerate(subs):
        start(UP, sub, here, above)
        start(DOWN, sub, here, below)
        start(X, sub, here)
        start(Y, (second + first)[k], here)
    swap_up.start()
    for number in range(chunks):
        stage_copy(number).wait()
        down[0, :, pl.ds(number * chunk, chunk)] = stage[number % 2].T
        if number + 2 < chunks:
            stage_copy(number + 2).start()
        turn_copy(number).start()

    cross(first[0], second[0])
    column(1, subs[0], True)
    cross(first[1], second[1])
    for sub in subs[1:]:
        column(1, sub, True)
    for sub in subs:
        spread(sub, sides(1)[1])
    ready_same(0, 0)
    own_up.wait()
    swap_up.wait()
    for number in range(chunks):
        turn_copy(number).wait()
    compute(0)
    for sub in subs:
        corner_own(sub)
    for sub in subs[:2]:
        column(2, sub)
    ready_other(0, 1)
    compute(1)
    for sub in subs[2:]:
        column(2, sub)
    partial()
    gather(0, 1)
    weight_grad((0, 1), acc_up, gx, pg)
    weight_grad((0, 1), acc_down, sq, gc, 0, 1)
    ready_same(1, 2)
    compute(2)
    weight_grad((0, 1), acc_down, sq, gc, 1, 2)
    pl.semaphore_signal(free_sem, inc=1, device_id=sibling, device_id_type=MESH)
    for sub in subs:
        corner(1, sub)
    ready_other(1, 3)
    compute(3)
    for turn in (0, 1):
        for array in (2, 3):
            pair_copy(array, turn).wait_send()
    pl.semaphore_wait(free_sem, 1)
    for sub in subs[:2]:
        column(3, sub)
    gather(2, 3)
    weight_grad((2, 3), acc_up, gx, pg, 0, 1, 2)
    ready_same(2, 4)
    compute(4, 0, 1)
    column(3, subs[2])
    far_cross(subs[0])
    compute(4, 1, 2)
    column(3, subs[3])
    weight_grad((2, 3), acc_up, gx, pg, 1, 2, 2)
    far_cross(subs[1])
    weight_grad((2, 3), acc_down, sq, gc)
    far_cross(subs[2])
    gather(4)
    weight_grad((4,), acc_up, gx, pg)
    weight_grad((4,), acc_down, sq, gc)
    far_cross(subs[3])
    part_copy.start()
    ready_same(3, 5)
    compute(5)
    for sub in subs:
        corner(2, sub)
    ready_other(2, 6)
    compute(6)
    ready_other(3, 7)
    compute(7)
    gather(5)
    weight_grad((5,), acc_up, gx, pg)
    weight_grad((5,), acc_down, sq, gc)
    gather(6, 7)
    part_copy.wait()
    for way, sub, at, condition in started:
        if condition is None:
            copy(way, sub, at).wait_send()
        else:
            pl.when(condition)(functools.partial(lambda w, s, a: copy(w, s, a).wait_send(), way, sub, at))
    for turn in range(len(turns)):
        for array in range(4):
            if array < 2 or turn >= 2:
                pair_copy(array, turn).wait_send()


def finish_kernel(reps, acc_up, acc_down, gx, gc, pg, sq, mine, theirs,
                  inputs_out, up_out, down_out, tiles, added, tile_sem, added_sem):
    rep = lax.axis_index("rep")
    z, y = rep // PAIR, rep % PAIR
    depth = reps // PAIR
    units = [nearest(z, depth, index) * PAIR + (1 - y) for index in (depth - 2, depth - 1)]
    height = gx.shape[2]
    slots, span, wide = tiles.shape
    tile = 256

    added[...] = (mine[...].astype(jnp.float32) + theirs[...].astype(jnp.float32)).astype(added.dtype)
    put = pltpu.make_async_copy(added, inputs_out, added_sem)
    put.start()

    def both(ref, unit, cols):
        block = ref[unit, pl.ds(OWN, 2), :, cols]
        return block.reshape(2 * height, block.shape[2])

    started = []
    for held, out, left, right in ((acc_up, up_out, gx, pg), (acc_down, down_out, sq, gc)):
        rows, cols = held.shape
        pairs = list(zip(*((units, PLACES[-2:]) if right is pg else (PLACES[-2:], units))))
        for at in (pl.ds(start, span) for start in range(0, rows, span)):
            lefts = [both(left, one, at) for one, _ in pairs]
            for begin in range(0, cols, wide):
                slot = len(started) % slots
                if len(started) >= slots:
                    started[-slots].wait()
                for start in range(0, wide, tile):
                    across = pl.ds(begin + start, tile)
                    total = sum(contract_rows(one, both(right, other, across)) for one, (_, other) in zip(lefts, pairs))
                    tiles[slot, :, pl.ds(start, tile)] = held[at, across] + total
                started.append(pltpu.make_async_copy(tiles.at[slot], out.at[at, pl.ds(begin, wide)], tile_sem.at[slot]))
                started[-1].start()
    for moved in started[-slots:]:
        moved.wait()
    put.wait()


def few_tokens(reps, inputs, cotangent, w_up, w_down):
    height, width = inputs.shape
    hidden = w_up.shape[1]
    depth = reps // PAIR
    low, high = inputs.dtype, jnp.float32
    far, vmem = pl.BlockSpec(memory_space=pltpu.HBM), pl.BlockSpec(memory_space=pltpu.VMEM)
    blocks, rows = (reps, 3, height, width), (max(PLACES) + 1, 2, height, hidden)
    shapes = [(w_up.shape, high), (w_down.shape, high), (blocks, low), (blocks, low), (rows, low), (rows, low),
              (inputs.shape, low), (inputs.shape, low)]
    chunk = w_down.shape[0] // 8
    tokens = reps * height
    held = pl.pallas_call(
        functools.partial(hidden_kernel, reps),
        out_shape=[pltpu.VMEM(shape, dtype) for shape, dtype in shapes],
        in_specs=[far] * 4,
        out_specs=[vmem] * len(shapes),
        scratch_shapes=[
            pltpu.VMEM((2,) + w_up.shape, low),
            pltpu.VMEM((2, width, hidden), low),
            pltpu.VMEM((2, chunk, width), low),
            pltpu.VMEM(inputs.shape, low),
            pltpu.SemaphoreType.REGULAR,
            pltpu.SemaphoreType.DMA((4, 4, reps * 2)),
            pltpu.SemaphoreType.DMA((4, reps * 2)),
            pltpu.SemaphoreType.DMA((2,)),
            pltpu.SemaphoreType.DMA((2, 8)),
            pltpu.SemaphoreType.DMA((3,)),
            pltpu.SemaphoreType.DMA((2,)),
            pltpu.SemaphoreType.DMA((4, reps)),
            pltpu.SemaphoreType.DMA((4, reps)),
            pltpu.SemaphoreType.DMA((2,)),
        ],
        cost_estimate=pl.CostEstimate(flops=14 * tokens * width * hidden, bytes_accessed=w_up.size * 8, transcendentals=0),
        compiler_params=pltpu.CompilerParams(
            collective_id=0, has_side_effects=True, vmem_limit_bytes=GRANT
        ),
    )(*(pltpu.with_memory_space_constraint(value, pltpu.HBM) for value in (inputs, cotangent, w_up, w_down)))
    return pl.pallas_call(
        functools.partial(finish_kernel, reps),
        out_shape=[
            jax.ShapeDtypeStruct(inputs.shape, low),
            jax.ShapeDtypeStruct(w_up.shape, high),
            jax.ShapeDtypeStruct(w_down.shape, high),
        ],
        in_specs=[vmem] * len(shapes),
        out_specs=[far] * 3,
        scratch_shapes=[
            pltpu.VMEM((4, width, width // 2), high),
            pltpu.VMEM(inputs.shape, low),
            pltpu.SemaphoreType.DMA((4,)),
            pltpu.SemaphoreType.DMA,
        ],
        cost_estimate=pl.CostEstimate(flops=16 * height * width * hidden, bytes_accessed=w_up.size * 16, transcendentals=0),
        compiler_params=pltpu.CompilerParams(vmem_limit_bytes=GRANT),
    )(*(pltpu.with_memory_space_constraint(value, pltpu.VMEM) for value in held))


def many_tokens(inputs, cotangent, w_up, w_down):
    rows_in, rows_cot = (
        lax.all_gather(inputs, "tp", axis=1, tiled=True),
        lax.all_gather(cotangent, "tp", axis=1, tiled=True),
    )
    cols_in, cols_cot = (
        lax.all_to_all(rows_in, "fs", split_axis=1, concat_axis=0, tiled=True),
        lax.all_to_all(rows_cot, "fs", split_axis=1, concat_axis=0, tiled=True),
    )
    full_up, full_down = (
        lax.all_gather(w_up, "fs", axis=0, tiled=True),
        lax.all_gather(w_down, "fs", axis=1, tiled=True),
    )
    act_grad = contract_cols(rows_cot, full_down)
    preact = jnp.dot(rows_in, full_up, preferred_element_type=jnp.float32)
    relu_pre = jnp.maximum(preact, 0.0)
    squared = (relu_pre * relu_pre).astype(jnp.bfloat16)
    pre_grad = (2.0 * relu_pre * act_grad).astype(jnp.bfloat16)
    partial_value = contract_cols(pre_grad, full_up)
    grad_inputs = lax.psum_scatter(
        partial_value.astype(jnp.bfloat16), "tp", scatter_dimension=1, tiled=True
    )
    grad_piece = lax.all_gather(pre_grad, "fs", axis=0, tiled=True)
    square_piece = lax.all_gather(squared, "fs", axis=0, tiled=True)
    local_up = contract_rows(cols_in, grad_piece)
    local_down = contract_rows(square_piece, cols_cot)
    slice_up = lax.psum_scatter(local_up, "rep", scatter_dimension=0, tiled=True)
    slice_down = lax.psum_scatter(local_down, "rep", scatter_dimension=0, tiled=True)
    grad_up = lax.all_gather(slice_up, "rep", axis=0, tiled=True)
    grad_down = lax.all_gather(slice_down, "rep", axis=0, tiled=True)
    return (grad_inputs, grad_up, grad_down)


def solution(mesh):
    reps, n_fs, n_tp = mesh.shape["rep"], mesh.shape["fs"], mesh.shape["tp"]

    def shards(inputs, cotangent, w_up, w_down):
        gathered = 2 * reps * n_tp * inputs.size * inputs.dtype.itemsize
        gradients = (w_up.size + w_down.size) * 4
        fits = n_fs == 2 and n_tp == 2 and reps == PAIR * 4 and inputs.shape[0] % 32 == 0
        if fits and gathered <= gradients:
            return few_tokens(reps, inputs, cotangent, w_up, w_down)
        return many_tokens(inputs, cotangent, w_up, w_down)

    return jax.shard_map(
        shards,
        mesh=mesh,
        in_specs=(P(("rep", "fs"), "tp"), P(("rep", "fs"), "tp"), P("fs", "tp"), P("tp", "fs")),
        out_specs=(P(("rep", "fs"), "tp"), P("fs", "tp"), P("tp", "fs")),
        check_vma=False,
    )
```

```python
import functools

import jax
import jax.numpy as jnp
from jax import lax
from jax.experimental import pallas as pl
from jax.experimental.pallas import tpu as pltpu
from jax.sharding import PartitionSpec as P

MESH = pl.DeviceIdType.MESH
X, Y, UP, DOWN = range(4)
PAIR = 2
OWN, SIBLING, OTHER = range(3)
PLACES = (0, 1, 2, 3, 0, 1, 4, 5)
GRANT = 22 * 1024 * 1024


def contract_rows(left, right):
    return lax.dot_general(
        left, right, (((0,), (0,)), ((), ())), preferred_element_type=jnp.float32
    )


def contract_cols(left, right):
    return lax.dot_general(
        left, right, (((1,), (1,)), ((), ())), preferred_element_type=jnp.float32
    )


def nearest(z, depth, index):
    near = jnp.minimum(z, depth - 1 - z)
    away = (index + 1) // 2
    around = z - away if index % 2 else z + away
    outward = jnp.where(z < depth - 1 - z, z + (index - near), z - (index - near))
    return jnp.where(index <= 2 * near, around, outward)


def hidden_kernel(reps, x_ref, c_ref, up_ref, down_ref,
                  acc_up, acc_down, gx, gc, pg, sq, mine, theirs,
                  up, down, stage, sent,
                  free_sem, send_sem, recv_sem, swap_sem, turn_sem, own_sem, stage_sem,
                  pair_send, pair_recv, part_sem):
    rep, fs, tp = lax.axis_index("rep"), lax.axis_index("fs"), lax.axis_index("tp")
    z, y = rep // PAIR, rep % PAIR
    depth = reps // PAIR
    height, width = x_ref.shape
    half = height // 2
    hidden = up.shape[2]
    reach = depth - 2
    target = {
        X: {"tp": 1 - tp},
        Y: {"rep": z * PAIR + (1 - y)},
        UP: {"rep": jnp.minimum(z + 1, depth - 1) * PAIR + y},
        DOWN: {"rep": jnp.maximum(z - 1, 0) * PAIR + y},
    }
    sibling = {"fs": 1 - fs}
    above, below = z < depth - 1, z > 0
    planes = [nearest(z, depth, index) for index in range(depth)]
    own_block = ((tp + fs) % 2) * OTHER

    chunk = stage.shape[1]
    chunks = down_ref.shape[0] // chunk

    def stage_copy(number):
        rows = pl.ds(number * chunk, chunk)
        return pltpu.make_async_copy(down_ref.at[rows], stage.at[number % 2], stage_sem.at[number % 2])

    owns = [
        pltpu.make_async_copy(x_ref, gx.at[rep, own_block], own_sem.at[0]),
        pltpu.make_async_copy(c_ref, gc.at[rep, own_block], own_sem.at[1]),
    ]
    for own in owns:
        own.start()
    stage_copy(0).start()
    stage_copy(1).start()
    own_up = pltpu.make_async_copy(up_ref, up.at[0], own_sem.at[2])
    own_up.start()

    barrier = pltpu.get_barrier_semaphore()

    def greet(device):
        pl.semaphore_signal(barrier, inc=1, device_id=device, device_id_type=MESH)

    greet(target[X])
    greet(target[Y])
    greet(sibling)
    pl.when(above)(lambda: greet(target[UP]))
    pl.when(below)(lambda: greet(target[DOWN]))
    pl.semaphore_wait(barrier, 3 + above.astype(jnp.int32) + below.astype(jnp.int32))

    started = []

    def copy(way, sub, at):
        at_z, at_y, at_t = at
        array, part = sub
        unit = at_z * PAIR + at_y
        place = (gx, gc)[array].at[unit, ((at_t + fs) % 2) * OTHER, pl.ds(part * half, half)]
        index, piece = array * 2 + part, unit * 2 + at_t
        return pltpu.make_async_remote_copy(
            src_ref=place, dst_ref=place,
            send_sem=send_sem.at[way, index, piece], recv_sem=recv_sem.at[index, piece],
            device_id=target[way], device_id_type=MESH,
        )

    def start(way, sub, at, condition=None):
        if condition is None:
            copy(way, sub, at).start()
        else:
            pl.when(condition)(lambda: copy(way, sub, at).start())
        started.append((way, sub, at, condition))

    def arrive(sub, at, condition=None):
        if condition is None:
            copy(X, sub, at).wait_recv()
        else:
            pl.when(condition)(lambda: copy(X, sub, at).wait_recv())

    first = [(array, 0) for array in range(2)]
    second = [(array, 1) for array in range(2)]
    subs = first + second
    far_y, far_x = first, second

    def sides(distance):
        return (
            (z - distance, z >= distance, UP, jnp.logical_and(z >= distance, above)),
            (z + distance, z + distance < depth, DOWN, jnp.logical_and(z + distance < depth, below)),
        )

    def spread(sub, side):
        at_z, there, _, _ = side
        start(X, sub, (at_z, y, tp), there)
        start(Y, sub, (at_z, y, tp), there)

    def column(distance, sub, defer=False):
        for side in sides(distance):
            at_z, there, way, onward = side
            arrive(sub, (at_z, y, tp), there)
            start(way, sub, (at_z, y, tp), onward)
            if way == UP or not defer:
                spread(sub, side)

    def cross(one, two):
        arrive(one, (z, y, 1 - tp))
        start(Y, one, (z, y, 1 - tp))
        arrive(two, (z, 1 - y, tp))
        start(X, two, (z, 1 - y, tp))

    def corner_own(sub):
        at = (z, 1 - y, 1 - tp)
        arrive(sub, at)
        start(UP, sub, at, above)
        start(DOWN, sub, at, below)

    def corner(distance, sub):
        for at_z, there, way, onward in sides(distance):
            at = (at_z, 1 - y, 1 - tp)
            arrive(sub, at, there)
            if distance < reach:
                start(way, sub, at, onward)

    last = planes[depth - 1]
    far = jnp.logical_or(last - z > reach, z - last > reach)

    def far_cross(sub):
        if sub in far_y:
            arrive(sub, (last, y, 1 - tp))
            start(Y, sub, (last, y, 1 - tp), far)
        else:
            arrive(sub, (last, 1 - y, tp))
            start(X, sub, (last, 1 - y, tp), far)

    def unit_of(index, row):
        return planes[index] * PAIR + row

    turns = [(0, y), (0, 1 - y), (1, y), (1, 1 - y), (2, y), (3, y), (2, 1 - y), (3, 1 - y)]

    def pair_copy(array, turn):
        held = (gx, gc, pg, sq)[array]
        at, source = (unit_of(*turns[turn]), OTHER) if array < 2 else (PLACES[turn], OWN)
        return pltpu.make_async_remote_copy(
            src_ref=held.at[at, source], dst_ref=held.at[at, SIBLING],
            send_sem=pair_send.at[array, turn], recv_sem=pair_recv.at[array, turn],
            device_id=sibling, device_id_type=MESH,
        )

    def ready_same(index, turn):
        done = first if index == 0 else far_y if index == depth - 1 else []
        for sub in subs:
            if sub not in done:
                arrive(sub, (planes[index], y, 1 - tp))
        for array in range(2):
            pair_copy(array, turn).start()

    def ready_other(index, turn):
        done = second if index == 0 else far_x if index == depth - 1 else []
        for sub in subs:
            if sub not in done:
                arrive(sub, (planes[index], 1 - y, tp))
        if index == depth - 1:
            for sub in subs:
                arrive(sub, (last, 1 - y, 1 - tp), far)
        for array in range(2):
            pair_copy(array, turn).start()

    def compute(turn, lo=0, hi=2):
        unit, place = unit_of(*turns[turn]), PLACES[turn]
        tile = hidden // 2

        @pl.loop(lo, hi)
        def _(step):
            cols = pl.ds(pl.multiple_of(step * tile, tile), tile)
            preact = (
                jnp.dot(gx[unit, OWN], up[0, :, cols], preferred_element_type=jnp.float32)
                + jnp.dot(gx[unit, OTHER], up[1, :, cols], preferred_element_type=jnp.float32)
            )
            act_grad = (
                jnp.dot(gc[unit, OWN], down[0, :, cols], preferred_element_type=jnp.float32)
                + jnp.dot(gc[unit, OTHER], down[1, :, cols], preferred_element_type=jnp.float32)
            )
            relu_pre = jnp.maximum(preact, 0.0)
            sq[place, OWN, :, cols] = (relu_pre * relu_pre).astype(sq.dtype)
            pg[place, OWN, :, cols] = (2.0 * relu_pre * act_grad).astype(pg.dtype)

        if hi == 2:
            for array in (2, 3):
                pair_copy(array, turn).start()

    def both(ref, unit, cols):
        block = ref[unit, pl.ds(OWN, 2), :, cols]
        return block.reshape(2 * height, block.shape[2])

    def gather(*several):
        for turn in several:
            for array in range(4):
                pair_copy(array, turn).wait_recv()

    def weight_grad(several, into, left, right, lo=0, hi=None, parts=1):
        rows, cols = into.shape
        span, tile = width // parts, 256

        def block(ref, turn, cols):
            return both(ref, unit_of(*turns[turn]) if ref is gx or ref is gc else PLACES[turn], cols)

        @pl.loop(lo, rows // span if hi is None else hi)
        def _(step):
            at = pl.ds(pl.multiple_of(step * span, span), span)
            lefts = [block(left, turn, at) for turn in several]
            for number in range(cols // tile):
                across = pl.ds(number * tile, tile)
                total = sum(contract_rows(one, block(right, turn, across)) for one, turn in zip(lefts, several))
                into[at, across] = total if 0 in several else into[at, across] + total

    def partial():
        tile = width // 4

        @pl.loop(0, width // tile)
        def _(step):
            cols = pl.ds(pl.multiple_of(step * tile, tile), tile)
            for slot, into in (((tp + fs) % 2, mine), ((tp + fs + 1) % 2, sent)):
                into[:, cols] = contract_cols(pg[PLACES[0], OWN], up[slot, cols, :]).astype(into.dtype)

    part_copy = pltpu.make_async_remote_copy(
        src_ref=sent, dst_ref=theirs, send_sem=part_sem.at[0], recv_sem=part_sem.at[1],
        device_id=target[X], device_id_type=MESH,
    )
    swap_up = pltpu.make_async_remote_copy(
        src_ref=up_ref, dst_ref=up.at[1], send_sem=swap_sem.at[0], recv_sem=swap_sem.at[1],
        device_id=sibling, device_id_type=MESH,
    )

    def turn_copy(number):
        cols = pl.ds(number * chunk, chunk)
        return pltpu.make_async_remote_copy(
            src_ref=down.at[0, :, cols], dst_ref=down.at[1, :, cols],
            send_sem=turn_sem.at[0, number], recv_sem=turn_sem.at[1, number],
            device_id=sibling, device_id_type=MESH,
        )

    for own in owns:
        own.wait()
    here = (z, y, tp)
    for k, sub in enumerate(subs):
        start(UP, sub, here, above)
        start(DOWN, sub, here, below)
        start(X, sub, here)
        start(Y, (second + first)[k], here)
    swap_up.start()
    for number in range(chunks):
        stage_copy(number).wait()
        down[0, :, pl.ds(number * chunk, chunk)] = stage[number % 2].T
        if number + 2 < chunks:
            stage_copy(number + 2).start()
        turn_copy(number).start()

    cross(first[0], second[0])
    column(1, subs[0], True)
    cross(first[1], second[1])
    for sub in subs[1:]:
        column(1, sub, True)
    for sub in subs:
        spread(sub, sides(1)[1])
    ready_same(0, 0)
    own_up.wait()
    swap_up.wait()
    for number in range(chunks):
        turn_copy(number).wait()
    compute(0)
    for sub in subs:
        corner_own(sub)
    for sub in subs[:2]:
        column(2, sub)
    ready_other(0, 1)
    compute(1)
    for sub in subs[2:]:
        column(2, sub)
    partial()
    gather(0, 1)
    weight_grad((0, 1), acc_up, gx, pg)
    weight_grad((0, 1), acc_down, sq, gc, 0, 1)
    ready_same(1, 2)
    compute(2)
    weight_grad((0, 1), acc_down, sq, gc, 1, 2)
    pl.semaphore_signal(free_sem, inc=1, device_id=sibling, device_id_type=MESH)
    for sub in subs:
        corner(1, sub)
    ready_other(1, 3)
    compute(3)
    for turn in (0, 1):
        for array in (2, 3):
            pair_copy(array, turn).wait_send()
    pl.semaphore_wait(free_sem, 1)
    for sub in subs[:2]:
        column(3, sub)
    gather(2, 3)
    weight_grad((2, 3), acc_up, gx, pg, 0, 1, 2)
    ready_same(2, 4)
    compute(4, 0, 1)
    column(3, subs[2])
    far_cross(subs[0])
    compute(4, 1, 2)
    column(3, subs[3])
    weight_grad((2, 3), acc_up, gx, pg, 1, 2, 2)
    far_cross(subs[1])
    weight_grad((2, 3), acc_down, sq, gc)
    far_cross(subs[2])
    gather(4)
    weight_grad((4,), acc_up, gx, pg)
    weight_grad((4,), acc_down, sq, gc)
    far_cross(subs[3])
    part_copy.start()
    ready_same(3, 5)
    compute(5)
    for sub in subs:
        corner(2, sub)
    ready_other(2, 6)
    compute(6)
    gather(5)
    weight_grad((5,), acc_up, gx, pg, 0, 1, 2)
    ready_other(3, 7)
    compute(7)
    weight_grad((5,), acc_up, gx, pg, 1, 2, 2)
    weight_grad((5,), acc_down, sq, gc)
    gather(6, 7)
    part_copy.wait()
    for way, sub, at, condition in started:
        if condition is None:
            copy(way, sub, at).wait_send()
        else:
            pl.when(condition)(functools.partial(lambda w, s, a: copy(w, s, a).wait_send(), way, sub, at))
    for turn in range(len(turns)):
        for array in range(4):
            if array < 2 or turn >= 2:
                pair_copy(array, turn).wait_send()


def finish_kernel(reps, acc_up, acc_down, gx, gc, pg, sq, mine, theirs,
                  inputs_out, up_out, down_out, tiles, added, tile_sem, added_sem):
    rep = lax.axis_index("rep")
    z, y = rep // PAIR, rep % PAIR
    depth = reps // PAIR
    units = [nearest(z, depth, index) * PAIR + (1 - y) for index in (depth - 2, depth - 1)]
    height = gx.shape[2]
    slots, span, wide = tiles.shape
    tile = 256

    added[...] = (mine[...].astype(jnp.float32) + theirs[...].astype(jnp.float32)).astype(added.dtype)
    put = pltpu.make_async_copy(added, inputs_out, added_sem)
    put.start()

    def both(ref, unit, cols):
        block = ref[unit, pl.ds(OWN, 2), :, cols]
        return block.reshape(2 * height, block.shape[2])

    started = []
    for held, out, left, right in ((acc_up, up_out, gx, pg), (acc_down, down_out, sq, gc)):
        rows, cols = held.shape
        pairs = list(zip(*((units, PLACES[-2:]) if right is pg else (PLACES[-2:], units))))
        for at in (pl.ds(start, span) for start in range(0, rows, span)):
            lefts = [both(left, one, at) for one, _ in pairs]
            for begin in range(0, cols, wide):
                slot = len(started) % slots
                if len(started) >= slots:
                    started[-slots].wait()
                for start in range(0, wide, tile):
                    across = pl.ds(begin + start, tile)
                    total = sum(contract_rows(one, both(right, other, across)) for one, (_, other) in zip(lefts, pairs))
                    tiles[slot, :, pl.ds(start, tile)] = held[at, across] + total
                started.append(pltpu.make_async_copy(tiles.at[slot], out.at[at, pl.ds(begin, wide)], tile_sem.at[slot]))
                started[-1].start()
    for moved in started[-slots:]:
        moved.wait()
    put.wait()


def few_tokens(reps, inputs, cotangent, w_up, w_down):
    height, width = inputs.shape
    hidden = w_up.shape[1]
    depth = reps // PAIR
    low, high = inputs.dtype, jnp.float32
    far, vmem = pl.BlockSpec(memory_space=pltpu.HBM), pl.BlockSpec(memory_space=pltpu.VMEM)
    blocks, rows = (reps, 3, height, width), (max(PLACES) + 1, 2, height, hidden)
    shapes = [(w_up.shape, high), (w_down.shape, high), (blocks, low), (blocks, low), (rows, low), (rows, low),
              (inputs.shape, low), (inputs.shape, low)]
    chunk = w_down.shape[0] // 8
    tokens = reps * height
    held = pl.pallas_call(
        functools.partial(hidden_kernel, reps),
        out_shape=[pltpu.VMEM(shape, dtype) for shape, dtype in shapes],
        in_specs=[far] * 4,
        out_specs=[vmem] * len(shapes),
        scratch_shapes=[
            pltpu.VMEM((2,) + w_up.shape, low),
            pltpu.VMEM((2, width, hidden), low),
            pltpu.VMEM((2, chunk, width), low),
            pltpu.VMEM(inputs.shape, low),
            pltpu.SemaphoreType.REGULAR,
            pltpu.SemaphoreType.DMA((4, 4, reps * 2)),
            pltpu.SemaphoreType.DMA((4, reps * 2)),
            pltpu.SemaphoreType.DMA((2,)),
            pltpu.SemaphoreType.DMA((2, 8)),
            pltpu.SemaphoreType.DMA((3,)),
            pltpu.SemaphoreType.DMA((2,)),
            pltpu.SemaphoreType.DMA((4, reps)),
            pltpu.SemaphoreType.DMA((4, reps)),
            pltpu.SemaphoreType.DMA((2,)),
        ],
        cost_estimate=pl.CostEstimate(flops=14 * tokens * width * hidden, bytes_accessed=w_up.size * 8, transcendentals=0),
        compiler_params=pltpu.CompilerParams(
            collective_id=0, has_side_effects=True, vmem_limit_bytes=GRANT
        ),
    )(*(pltpu.with_memory_space_constraint(value, pltpu.HBM) for value in (inputs, cotangent, w_up, w_down)))
    return pl.pallas_call(
        functools.partial(finish_kernel, reps),
        out_shape=[
            jax.ShapeDtypeStruct(inputs.shape, low),
            jax.ShapeDtypeStruct(w_up.shape, high),
            jax.ShapeDtypeStruct(w_down.shape, high),
        ],
        in_specs=[vmem] * len(shapes),
        out_specs=[far] * 3,
        scratch_shapes=[
            pltpu.VMEM((4, width, width // 2), high),
            pltpu.VMEM(inputs.shape, low),
            pltpu.SemaphoreType.DMA((4,)),
            pltpu.SemaphoreType.DMA,
        ],
        cost_estimate=pl.CostEstimate(flops=16 * height * width * hidden, bytes_accessed=w_up.size * 16, transcendentals=0),
        compiler_params=pltpu.CompilerParams(vmem_limit_bytes=GRANT),
    )(*(pltpu.with_memory_space_constraint(value, pltpu.VMEM) for value in held))


def many_tokens(inputs, cotangent, w_up, w_down):
    rows_in, rows_cot = (
        lax.all_gather(inputs, "tp", axis=1, tiled=True),
        lax.all_gather(cotangent, "tp", axis=1, tiled=True),
    )
    cols_in, cols_cot = (
        lax.all_to_all(rows_in, "fs", split_axis=1, concat_axis=0, tiled=True),
        lax.all_to_all(rows_cot, "fs", split_axis=1, concat_axis=0, tiled=True),
    )
    full_up, full_down = (
        lax.all_gather(w_up, "fs", axis=0, tiled=True),
        lax.all_gather(w_down, "fs", axis=1, tiled=True),
    )
    act_grad = contract_cols(rows_cot, full_down)
    preact = jnp.dot(rows_in, full_up, preferred_element_type=jnp.float32)
    relu_pre = jnp.maximum(preact, 0.0)
    squared = (relu_pre * relu_pre).astype(jnp.bfloat16)
    pre_grad = (2.0 * relu_pre * act_grad).astype(jnp.bfloat16)
    partial_value = contract_cols(pre_grad, full_up)
    grad_inputs = lax.psum_scatter(
        partial_value.astype(jnp.bfloat16), "tp", scatter_dimension=1, tiled=True
    )
    grad_piece = lax.all_gather(pre_grad, "fs", axis=0, tiled=True)
    square_piece = lax.all_gather(squared, "fs", axis=0, tiled=True)
    local_up = contract_rows(cols_in, grad_piece)
    local_down = contract_rows(square_piece, cols_cot)
    slice_up = lax.psum_scatter(local_up, "rep", scatter_dimension=0, tiled=True)
    slice_down = lax.psum_scatter(local_down, "rep", scatter_dimension=0, tiled=True)
    grad_up = lax.all_gather(slice_up, "rep", axis=0, tiled=True)
    grad_down = lax.all_gather(slice_down, "rep", axis=0, tiled=True)
    return (grad_inputs, grad_up, grad_down)


def solution(mesh):
    reps, n_fs, n_tp = mesh.shape["rep"], mesh.shape["fs"], mesh.shape["tp"]

    def shards(inputs, cotangent, w_up, w_down):
        gathered = 2 * reps * n_tp * inputs.size * inputs.dtype.itemsize
        gradients = (w_up.size + w_down.size) * 4
        fits = n_fs == 2 and n_tp == 2 and reps == PAIR * 4 and inputs.shape[0] % 32 == 0
        if fits and gathered <= gradients:
            return few_tokens(reps, inputs, cotangent, w_up, w_down)
        return many_tokens(inputs, cotangent, w_up, w_down)

    return jax.shard_map(
        shards,
        mesh=mesh,
        in_specs=(P(("rep", "fs"), "tp"), P(("rep", "fs"), "tp"), P("fs", "tp"), P("tp", "fs")),
        out_specs=(P(("rep", "fs"), "tp"), P("fs", "tp"), P("tp", "fs")),
        check_vma=False,
    )
```
